32 devices in a mesh: sp: 4 (over z), fs: 4 (over y, core), tp: 2 (over x).
Axes of the slice: x: 2, y: 2, z: 4, core: 2. Of those that a mesh axis runs over, the one named last changes fastest.
Arguments:
- tokens: bfloat16 [4, 4096, 2048], P('fs', 'sp', 'tp'), may hold values from -8 to 8
- norm_gain: float32 [2048], replicated, may hold values from 0.1 to 1.9
- w_query: bfloat16 [2048, 1024], P(('sp', 'fs'), 'tp'), may hold values from -4 to 4
- w_key: bfloat16 [2048, 512], P(('sp', 'fs'), 'tp'), may hold values from -0.16 to 0.16
- w_value: bfloat16 [2048, 512], P(('sp', 'fs'), 'tp'), may hold values from -0.125 to 0.125
- w_conv_in: bfloat16 [2048, 1024], P(('sp', 'fs'), 'tp'), may hold values from -0.125 to 0.125
- w_conv_b: bfloat16 [2048, 1024], P(('sp', 'fs'), 'tp'), may hold values from -0.125 to 0.125
- w_conv_c: bfloat16 [2048, 1024], P(('sp', 'fs'), 'tp'), may hold values from -0.125 to 0.125
- conv_taps: bfloat16 [3, 1024], P(None, 'tp'), may hold values from -3.5 to 3.5
- sink_logits: float32 [16], P('tp'), may hold values from 1 to 5
- w_attn_out: bfloat16 [1024, 2048], P('tp', ('sp', 'fs')), may hold values from -0.375 to 0.375
- w_conv_out: bfloat16 [1024, 2048], P('tp', ('sp', 'fs')), may hold values from -0.125 to 0.125
Outputs:
- mixed: bfloat16 [4, 4096, 2048], P('fs', ('sp', 'tp'))
The draws below stay inside these ranges and needn't reach their ends.
All inputs are finite; a program needn't handle non-finite values.
Results may differ from the reference program's by a relative error of at most 0.02.
Values may be sent and summed in bfloat16 or wider, within the bound.
A program may use at most 128 MiB of HBM per device.

```python
import jax
import jax.numpy as jnp
from jax import lax

D = 2048
HEADS = 16
KV_HEADS = 8
HEAD = 64
CONV = 1024
WINDOW = 128
SEQS = 4
LENGTH = 4096
N_TP = 2


def query_key_pair(key):
    folded = jax.random.fold_in(key, 11)
    first, second = jax.random.split(folded, 2)
    key_weights = jnp.clip(jax.random.normal(first, (D, KV_HEADS * HEAD), jnp.float32) * D ** (-0.5), -0.15, 0.15)
    query_weights = jax.random.normal(second, (D, HEADS * HEAD), jnp.float32) * D ** (-0.5)
    query_weights = jnp.clip(query_weights, -4.0, 4.0)
    return (query_weights, key_weights)


def draw_w_query(key, part):
    return query_key_pair(key)[0].astype(jnp.bfloat16)


def draw_w_key(key, part):
    return query_key_pair(key)[1].astype(jnp.bfloat16)


def draw_tokens(key, part):
    folded = jax.random.fold_in(key, 23)
    first = jax.random.fold_in(folded, 0)
    values = jax.random.normal(first, (SEQS, LENGTH, D), jnp.float32)
    return jnp.clip(values, -8.0, 8.0).astype(jnp.bfloat16)


def block_levels(own_key, extent, shards, least, top_value):
    def one(axis_at, shards_of):
        heights = jax.random.uniform(jax.random.fold_in(jax.random.fold_in(own_key, 6), axis_at), (shards_of,), jnp.float32, least / len(shards), top_value / len(shards))
        return jnp.repeat(jnp.exp(heights), extent[axis_at] // shards_of).reshape((-1,) + (1,) * (len(extent) - axis_at - 1))

    gain = one(*shards[0])
    for cut in shards[1:]:
        gain = gain * one(*cut)
    return gain


def normal_values(key, dims, deviation, bound, shards=(), kind=jnp.bfloat16):
    entries = jax.random.normal(key, dims, jnp.float32) * deviation
    if len(shards) > 0:
        entries = block_levels(key, dims, shards, -0.22, 0.18) * entries
    return jnp.clip(entries, min=-bound, max=bound).astype(kind)


def setup_inputs(seed: int = 0) -> dict:
    key_list = jax.random.split(jax.random.key(seed), 13)
    return {
        "tokens": draw_tokens(jax.random.fold_in(key_list[12], 71), 0),
        "norm_gain": jnp.clip(1.0 + 0.18 * jax.random.normal(key_list[1], (D,), jnp.float32), 0.1, 1.9),
        "w_query": draw_w_query(jax.random.fold_in(key_list[12], 71), 0),
        "w_key": draw_w_key(jax.random.fold_in(key_list[12], 71), 0),
        "w_value": normal_values(key_list[4], (D, KV_HEADS * HEAD), D ** -0.5, 0.125, ((0, 16), (1, 2))),
        "w_conv_in": normal_values(key_list[5], (D, CONV), D ** -0.5, 0.125, ((0, 16), (1, 2))),
        "w_conv_b": normal_values(key_list[6], (D, CONV), D ** -0.5, 0.125, ((0, 16), (1, 2))),
        "w_conv_c": normal_values(key_list[7], (D, CONV), D ** -0.5, 0.125, ((0, 16), (1, 2))),
        "conv_taps": normal_values(key_list[8], (3, CONV), 3 ** -0.5, 3.5, ((1, 2),)),
        "sink_logits": jnp.clip(1.0 + 4.0 * jax.random.uniform(key_list[9], (HEADS,), jnp.float32) ** block_levels(key_list[9], (HEADS,), ((0, 2),), -0.2, 0.2), 1.0, 5.0),
        "w_attn_out": normal_values(key_list[10], (HEADS * HEAD, D), (D // 8) ** -0.5, 0.375, ((0, 2), (1, 16))),
        "w_conv_out": normal_values(key_list[11], (CONV, D), D ** -0.5, 0.125, ((0, 2), (1, 16))),
    }


def norm_rows(tokens, norm_gain):
    values = tokens.astype(jnp.float32)
    average = lax.optimization_barrier(jnp.mean(values, axis=-1, keepdims=True))
    centred = values - average
    variance = lax.optimization_barrier(jnp.mean(centred * centred, axis=-1, keepdims=True))
    return (centred * lax.rsqrt(variance + 1e-05) * norm_gain.astype(jnp.float32)).astype(jnp.bfloat16)

def project(normed, weight):
    return jnp.dot(normed, weight, preferred_element_type=jnp.float32).astype(jnp.bfloat16)

def window_attention(queries, keys, values, sink_logits):
    length = queries.shape[0]
    blocks = length // WINDOW
    group = HEADS // KV_HEADS
    query_form = queries.astype(jnp.float32).reshape(blocks, WINDOW, KV_HEADS, group, HEAD)
    zero_rows = jnp.zeros((WINDOW, KV_HEADS * HEAD), jnp.bfloat16)
    padded_keys = jnp.concatenate([zero_rows, keys], axis=0).astype(jnp.float32).reshape(blocks + 1, WINDOW, KV_HEADS, HEAD)
    padded_values = jnp.concatenate([zero_rows, values], axis=0).astype(jnp.float32).reshape(blocks + 1, WINDOW, KV_HEADS, HEAD)
    band_keys = jnp.concatenate([padded_keys[:-1], padded_keys[1:]], axis=1)
    band_values = jnp.concatenate([padded_values[:-1], padded_values[1:]], axis=1)
    scores = jnp.einsum('bqkgd,bskd->bkgqs', query_form, band_keys) * HEAD ** (-0.5)
    row_ids = jnp.arange(WINDOW, dtype=jnp.int32)[:, None]
    col_ids = jnp.arange(2 * WINDOW, dtype=jnp.int32)[None, :]
    distance = WINDOW + row_ids - col_ids
    head_ids = jnp.arange(HEADS, dtype=jnp.int32).reshape(KV_HEADS, group)
    slopes = jnp.exp2(-8.0 * (head_ids + 1).astype(jnp.float32) / HEADS)
    scores = scores - slopes[:, :, None, None] * distance.astype(jnp.float32)
    key_place = jnp.arange(blocks, dtype=jnp.int32)[:, None] * WINDOW - WINDOW + jnp.arange(2 * WINDOW, dtype=jnp.int32)[None, :]
    inside = (distance >= 0) & (distance < WINDOW)
    keep = inside[None, None, None, :, :] & (key_place >= 0)[:, None, None, None, :]
    scores = jnp.where(keep, scores, -jnp.inf)
    sinks = sink_logits.astype(jnp.float32).reshape(KV_HEADS, group)[:, :, None, None]
    highest = jnp.maximum(lax.optimization_barrier(jnp.max(scores, axis=-1, keepdims=True)), sinks)
    raised = jnp.exp(scores - highest)
    denominator = lax.optimization_barrier(jnp.sum(raised, axis=-1, keepdims=True)) + jnp.exp(sinks - highest)
    weights = (raised / denominator).astype(jnp.bfloat16)
    mixed = jnp.einsum('bkgqs,bskd->bqkgd', weights.astype(jnp.float32), band_values)
    return mixed.astype(jnp.bfloat16).reshape(length, HEADS * HEAD)

def reference(tokens, norm_gain, w_query, w_key, w_value, w_conv_in, w_conv_b, w_conv_c, conv_taps, sink_logits, w_attn_out, w_conv_out):
    normed_all = norm_rows(tokens, norm_gain)
    head_cols = HEADS * HEAD // N_TP
    chan_cols = CONV // N_TP
    taps = conv_taps.astype(jnp.float32)

    def one_sequence(normed):
        queries = project(normed, w_query)
        keys = project(normed, w_key)
        values = project(normed, w_value)
        inner = project(normed, w_conv_in)
        gate_b = project(normed, w_conv_b)
        gate_c = project(normed, w_conv_c)
        attended = window_attention(queries, keys, values, sink_logits)
        product = (gate_c.astype(jnp.float32) * inner.astype(jnp.float32)).astype(jnp.bfloat16)
        padded = jnp.concatenate([jnp.zeros((2, CONV), jnp.float32), product.astype(jnp.float32)], axis=0)
        length = product.shape[0]
        filtered = taps[0] * padded[0:length] + taps[1] * padded[1:length + 1] + taps[2] * padded[2:length + 2]
        conv_out = (gate_b.astype(jnp.float32) * filtered).astype(jnp.bfloat16)
        summed = jnp.zeros((length, D), jnp.float32)
        for group_id in range(N_TP):
            head_slice = slice(group_id * head_cols, (group_id + 1) * head_cols)
            chan_slice = slice(group_id * chan_cols, (group_id + 1) * chan_cols)
            partial_sum = jnp.dot(attended[:, head_slice], w_attn_out[head_slice], preferred_element_type=jnp.float32)
            partial_sum = partial_sum + jnp.dot(conv_out[:, chan_slice], w_conv_out[chan_slice], preferred_element_type=jnp.float32)
            summed = summed + partial_sum.astype(jnp.bfloat16).astype(jnp.float32)
        return summed.astype(jnp.bfloat16)
    return lax.map(one_sequence, normed_all)
```

```python
import functools

import jax
import jax.numpy as jnp
from jax import lax
from jax.experimental import pallas as pl
from jax.experimental.pallas import tpu as pltpu
from jax.sharding import PartitionSpec as P

HEADS = 16
HEAD = 64
WINDOW = 128
MESH = pl.DeviceIdType.MESH
Z_FIRST = (True, False, True)


class Gather:
    def __init__(self, ring, fs, parts):
        self.ring, self.outer, self.parts = ring, fs // 2, parts

    def sends(self, part, key):
        d, o, i = key
        if i == 1:
            return []
        out = []
        heavy_right = (part // 2 + o) % 2 == 0
        right = self.ring // 2 if heavy_right else (self.ring - 1) // 2
        left = self.ring - 1 - right
        if Z_FIRST[part]:
            on_ring, on_outer = o == 0, o == 0
        else:
            on_ring, on_outer = True, o == 0 and d == 0
        if on_ring:
            if d < right:
                out.append(("right", (d + 1, o, 0)))
            if d == 0 and left > 0:
                out.append(("left", (self.ring - 1, o, 0)))
            elif d > right and self.ring - d < left:
                out.append(("left", (d - 1, o, 0)))
        if on_outer:
            for step in range(1, self.outer):
                out.append((("outer", step), (d, step, 0)))
        out.append(("core", (d, o, 1)))
        return out

    def plan(self):
        order, level = [], {}
        frontier = [(0, part, (0, 0, 0)) for part in range(self.parts)]
        while frontier:
            frontier.sort()
            hops, part, key = frontier.pop(0)
            order.append((part, key, self.sends(part, key)))
            for _, there in self.sends(part, key):
                frontier.append((hops + 1, part, there))
        return order


def gather_kernel(gather, n_tp, *refs):
    parts = gather.parts
    own = refs[:parts]
    tok = refs[parts]
    full = refs[parts + 1 : 2 * parts + 1]
    tok_full = refs[2 * parts + 1]
    send_sem, recv_sem, local_sem, tok_send, tok_recv = refs[2 * parts + 2 :]
    n_sp, n_out = gather.ring, gather.outer
    s, f, t = lax.axis_index("sp"), lax.axis_index("fs"), lax.axis_index("tp")
    o, i = f // 2, f % 2

    def device(where):
        if where == "right":
            return (lax.rem(s + 1, n_sp), f, t)
        if where == "left":
            return (lax.rem(s + n_sp - 1, n_sp), f, t)
        if where == "core":
            return (s, o * 2 + (1 - i), t)
        if where[0] == "outer":
            return (s, lax.rem(o + where[1], n_out) * 2 + i, t)
        return (s, f, lax.rem(t + where[1], n_tp))

    barrier = pltpu.get_barrier_semaphore()
    greeted = ["right", "left", "core"]
    greeted += [("outer", k) for k in range(1, n_out)] + [("tp", k) for k in range(1, n_tp)]
    for where in greeted:
        pl.semaphore_signal(barrier, inc=1, device_id=device(where), device_id_type=MESH)
    pl.semaphore_wait(barrier, len(greeted))

    def origin(key):
        d, od, c = key
        src_s = lax.rem(s + n_sp - d, n_sp)
        src_o = lax.rem(o + n_out - od, n_out)
        src_i = i if c == 0 else 1 - i
        return src_s * (2 * n_out) + src_o * 2 + src_i

    cols = tok.shape[1]
    tok_copies = []
    for k in range(1, n_tp):
        copy = pltpu.make_async_remote_copy(
            src_ref=tok,
            dst_ref=tok_full.at[:, pl.ds(pl.multiple_of(t * cols, cols), cols)],
            send_sem=tok_send.at[k],
            recv_sem=tok_recv.at[k],
            device_id=device(("tp", k)),
            device_id_type=MESH,
        )
        copy.start()
        tok_copies.append(copy)
    flat = lambda key: (key[0] * n_out + key[1]) * 2 + key[2]
    copies, arrived, last = [], {}, []
    for part, key, sends in gather.plan():
        rows = own[part].shape[0]
        place = full[part].at[pl.ds(pl.multiple_of(origin(key) * rows, rows), rows)]
        if key == (0, 0, 0):
            source = own[part]
        else:
            source = place
            if sends:
                arrived[(part, key)].wait_recv()
            else:
                last.append(arrived[(part, key)])
        for where, there in sends:
            copy = pltpu.make_async_remote_copy(
                src_ref=source,
                dst_ref=place,
                send_sem=send_sem.at[len(copies)],
                recv_sem=recv_sem.at[part * 2 * n_sp * n_out + flat(there)],
                device_id=device(where),
                device_id_type=MESH,
            )
            copy.start()
            copies.append(copy)
            arrived[(part, there)] = copy
    local = []
    for part in range(parts):
        rows = own[part].shape[0]
        mine = pl.ds(pl.multiple_of(origin((0, 0, 0)) * rows, rows), rows)
        local.append(pltpu.make_async_copy(own[part], full[part].at[mine], local_sem.at[part]))
    mine = pl.ds(pl.multiple_of(t * cols, cols), cols)
    local.append(pltpu.make_async_copy(tok, tok_full.at[:, mine], local_sem.at[parts]))
    for copy in local:
        copy.start()
    for copy in last:
        copy.wait_recv()
    for copy in tok_copies:
        copy.wait()
    for copy in copies:
        copy.wait_send()
    for copy in local:
        copy.wait()


def gather_all(tokens, blocks):
    n_sp, n_fs, n_tp = (lax.axis_size(axis) for axis in ("sp", "fs", "tp"))
    gather = Gather(n_sp, n_fs, len(blocks))
    number = sum(len(sends) for _, _, sends in gather.plan())
    shapes = [jax.ShapeDtypeStruct((n_sp * n_fs * b.shape[0], b.shape[1]), b.dtype) for b in blocks]
    shapes.append(jax.ShapeDtypeStruct((tokens.shape[0], tokens.shape[1] * n_tp), tokens.dtype))
    return pl.pallas_call(
        functools.partial(gather_kernel, gather, n_tp),
        out_shape=shapes,
        in_specs=[pl.BlockSpec(memory_space=pl.ANY)] * (len(blocks) + 1),
        out_specs=[pl.BlockSpec(memory_space=pl.ANY)] * len(shapes),
        scratch_shapes=[
            pltpu.SemaphoreType.DMA((number,)),
            pltpu.SemaphoreType.DMA((len(blocks) * n_sp * n_fs,)),
            pltpu.SemaphoreType.DMA((len(blocks) + 1,)),
            pltpu.SemaphoreType.DMA((n_tp,)),
            pltpu.SemaphoreType.DMA((n_tp,)),
        ],
        compiler_params=pltpu.CompilerParams(collective_id=0, has_side_effects=True),
    )(*blocks, tokens)


def shifted(block, axis, distance):
    devices = range(lax.axis_size(axis))
    route = [(i - distance, i) for i in devices if i - distance in devices]
    return lax.ppermute(block, axis, route)


def norm_rows(tokens, norm_gain):
    values = tokens.astype(jnp.float32)
    average = jnp.mean(values, axis=-1, keepdims=True)
    centred = values - average
    variance = jnp.mean(centred * centred, axis=-1, keepdims=True)
    return (centred * lax.rsqrt(variance + 1e-05) * norm_gain).astype(jnp.bfloat16)


def attend(queries, keys_values, earlier_rows, sink_logits, head_base, row_base):
    row_total = queries.shape[0]
    kv_cols = keys_values.shape[1] // 2
    kv_here = kv_cols // HEAD
    heads_here = queries.shape[1] // HEAD
    group = heads_here // kv_here
    keys_all = jnp.concatenate([earlier_rows, keys_values], axis=0)
    block_rows = min(512, row_total)
    head_ids = head_base + jnp.arange(heads_here, dtype=jnp.int32)
    slopes = jnp.exp2(-8.0 * (head_ids + 1).astype(jnp.float32) / HEADS).reshape(kv_here, group)[
        :, :, None, None
    ]
    sinks = sink_logits.reshape(kv_here, group)[:, :, None, None]
    row_ids = jnp.arange(block_rows, dtype=jnp.int32)[:, None]
    col_ids = jnp.arange(block_rows + WINDOW, dtype=jnp.int32)[None, :]
    distance = WINDOW + row_ids - col_ids
    outputs = []
    for block in range(row_total // block_rows):
        first_row = block * block_rows
        query_block = queries[first_row : first_row + block_rows].reshape(
            block_rows, kv_here, group, HEAD
        )
        band = keys_all[first_row : first_row + block_rows + WINDOW]
        band_keys = band[:, :kv_cols].reshape(block_rows + WINDOW, kv_here, HEAD)
        band_values = band[:, kv_cols:].reshape(block_rows + WINDOW, kv_here, HEAD)
        scores = jnp.einsum(
            "qkgd,skd->kgqs", query_block, band_keys, preferred_element_type=jnp.float32
        ) * HEAD ** (-0.5)
        scores = scores - slopes * distance.astype(jnp.float32)
        key_place = row_base + first_row - WINDOW + col_ids
        keep = (distance >= 0) & (distance < WINDOW) & (key_place >= 0)
        scores = jnp.where(keep, scores, -jnp.inf)
        highest = jnp.maximum(jnp.max(scores, axis=-1, keepdims=True), sinks)
        raised = jnp.exp(scores - highest)
        denominator = jnp.sum(raised, axis=-1, keepdims=True) + jnp.exp(sinks - highest)
        weights = (raised / denominator).astype(jnp.bfloat16)
        mixed = jnp.einsum(
            "kgqs,skd->qkgd", weights, band_values, preferred_element_type=jnp.float32
        )
        outputs.append(mixed.astype(jnp.bfloat16).reshape(block_rows, heads_here * HEAD))
    return jnp.concatenate(outputs, axis=0)


def on_device(
    tokens,
    norm_gain,
    w_query,
    w_key,
    w_value,
    w_conv_in,
    w_conv_b,
    w_conv_c,
    conv_taps,
    sink_logits,
    w_attn_out,
    w_conv_out,
):
    blocks = (
        jnp.concatenate([w_query, w_key, w_value], axis=1),
        jnp.concatenate([w_conv_in, w_conv_b, w_conv_c], axis=1),
        jnp.concatenate([w_attn_out, w_conv_out], axis=0).T,
    )
    w_qkv, w_conv, w_out, gathered = gather_all(tokens[0], blocks)
    normed = norm_rows(gathered, norm_gain)
    row_total = normed.shape[0]
    q_cols, kv_cols, conv_cols = w_query.shape[1], w_key.shape[1], w_conv_in.shape[1]
    qkv = jnp.dot(normed, w_qkv, preferred_element_type=jnp.float32).astype(jnp.bfloat16)
    conv = jnp.dot(normed, w_conv, preferred_element_type=jnp.float32).astype(jnp.bfloat16)
    queries, keys_values = qkv[:, :q_cols], qkv[:, q_cols:]
    inner, gate_b, gate_c = (conv[:, k * conv_cols : (k + 1) * conv_cols] for k in range(3))
    product = (gate_c.astype(jnp.float32) * inner.astype(jnp.float32)).astype(jnp.bfloat16)
    earlier_kv, earlier_product = shifted(
        (keys_values[row_total - WINDOW :], product[row_total - 2 :]), "sp", 1
    )
    heads_here = queries.shape[1] // HEAD
    head_base = lax.axis_index("tp") * heads_here
    row_base = lax.axis_index("sp") * row_total
    attended = attend(queries, keys_values, earlier_kv, sink_logits, head_base, row_base)
    taps = conv_taps.astype(jnp.float32)
    padded = jnp.concatenate([earlier_product, product], axis=0).astype(jnp.float32)
    filtered = (
        taps[0] * padded[0:row_total]
        + taps[1] * padded[1 : row_total + 1]
        + taps[2] * padded[2 : row_total + 2]
    )
    conv_out = (gate_b.astype(jnp.float32) * filtered).astype(jnp.bfloat16)
    mixers = jnp.concatenate([attended, conv_out], axis=1)
    partial = lax.dot_general(
        mixers, w_out, (((1,), (1,)), ((), ())), preferred_element_type=jnp.float32
    ).astype(jnp.bfloat16)
    summed = lax.psum_scatter(partial, "tp", scatter_dimension=0, tiled=True)
    return summed[None]


def solution(mesh):
    placed = (
        P("fs", "sp", "tp"),
        P(),
        P(("sp", "fs"), "tp"),
        P(("sp", "fs"), "tp"),
        P(("sp", "fs"), "tp"),
        P(("sp", "fs"), "tp"),
        P(("sp", "fs"), "tp"),
        P(("sp", "fs"), "tp"),
        P(None, "tp"),
        P("tp"),
        P("tp", ("sp", "fs")),
        P("tp", ("sp", "fs")),
    )
    return jax.shard_map(
        on_device,
        mesh=mesh,
        in_specs=placed,
        out_specs=P("fs", ("sp", "tp"), None),
        check_vma=False,
    )
```

```python
import functools

import jax
import jax.numpy as jnp
from jax import lax
from jax.experimental import pallas as pl
from jax.experimental.pallas import tpu as pltpu
from jax.sharding import PartitionSpec as P

HEADS = 16
HEAD = 64
WINDOW = 128
MESH = pl.DeviceIdType.MESH
Z_FIRST = (True, True, False, True)


class Gather:
    def __init__(self, ring, fs, parts):
        self.ring, self.outer, self.parts = ring, fs // 2, parts

    def sends(self, part, key):
        d, o, i = key
        if i == 1:
            return []
        out = []
        heavy_right = (part // 2 + o) % 2 == 0
        right = self.ring // 2 if heavy_right else (self.ring - 1) // 2
        left = self.ring - 1 - right
        if Z_FIRST[part]:
            on_ring, on_outer = o == 0, o == 0
        else:
            on_ring, on_outer = True, o == 0 and d == 0
        if on_ring:
            if d < right:
                out.append(("right", (d + 1, o, 0)))
            if d == 0 and left > 0:
                out.append(("left", (self.ring - 1, o, 0)))
            elif d > right and self.ring - d < left:
                out.append(("left", (d - 1, o, 0)))
        if on_outer:
            for step in range(1, self.outer):
                out.append((("outer", step), (d, step, 0)))
        out.append(("core", (d, o, 1)))
        return out

    def plan(self):
        order, level = [], {}
        frontier = [(0, part, (0, 0, 0)) for part in range(self.parts)]
        while frontier:
            frontier.sort()
            hops, part, key = frontier.pop(0)
            order.append((part, key, self.sends(part, key)))
            for _, there in self.sends(part, key):
                frontier.append((hops + 1, part, there))
        return order


def gather_kernel(gather, n_tp, *refs):
    parts = gather.parts
    own = refs[:parts]
    tok = refs[parts]
    full = refs[parts + 1 : 2 * parts + 1]
    tok_full = refs[2 * parts + 1]
    send_sem, recv_sem, local_sem, tok_send, tok_recv = refs[2 * parts + 2 :]
    n_sp, n_out = gather.ring, gather.outer
    s, f, t = lax.axis_index("sp"), lax.axis_index("fs"), lax.axis_index("tp")
    o, i = f // 2, f % 2

    def device(where):
        if where == "right":
            return (lax.rem(s + 1, n_sp), f, t)
        if where == "left":
            return (lax.rem(s + n_sp - 1, n_sp), f, t)
        if where == "core":
            return (s, o * 2 + (1 - i), t)
        if where[0] == "outer":
            return (s, lax.rem(o + where[1], n_out) * 2 + i, t)
        return (s, f, lax.rem(t + where[1], n_tp))

    barrier = pltpu.get_barrier_semaphore()
    greeted = ["right", "left", "core"]
    greeted += [("outer", k) for k in range(1, n_out)] + [("tp", k) for k in range(1, n_tp)]
    for where in greeted:
        pl.semaphore_signal(barrier, inc=1, device_id=device(where), device_id_type=MESH)
    pl.semaphore_wait(barrier, len(greeted))

    def origin(key):
        d, od, c = key
        src_s = lax.rem(s + n_sp - d, n_sp)
        src_o = lax.rem(o + n_out - od, n_out)
        src_i = i if c == 0 else 1 - i
        return src_s * (2 * n_out) + src_o * 2 + src_i

    cols = tok.shape[1]
    tok_copies = []
    for k in range(1, n_tp):
        copy = pltpu.make_async_remote_copy(
            src_ref=tok,
            dst_ref=tok_full.at[:, pl.ds(pl.multiple_of(t * cols, cols), cols)],
            send_sem=tok_send.at[k],
            recv_sem=tok_recv.at[k],
            device_id=device(("tp", k)),
            device_id_type=MESH,
        )
        copy.start()
        tok_copies.append(copy)
    flat = lambda key: (key[0] * n_out + key[1]) * 2 + key[2]
    copies, arrived, last = [], {}, []
    for part, key, sends in gather.plan():
        rows = own[part].shape[0]
        place = full[part].at[pl.ds(pl.multiple_of(origin(key) * rows, rows), rows)]
        if key == (0, 0, 0):
            source = own[part]
        else:
            source = place
            if sends:
                arrived[(part, key)].wait_recv()
            else:
                last.append(arrived[(part, key)])
        for where, there in sends:
            copy = pltpu.make_async_remote_copy(
                src_ref=source,
                dst_ref=place,
                send_sem=send_sem.at[len(copies)],
                recv_sem=recv_sem.at[part * 2 * n_sp * n_out + flat(there)],
                device_id=device(where),
                device_id_type=MESH,
            )
            copy.start()
            copies.append(copy)
            arrived[(part, there)] = copy
    local = []
    for part in range(parts):
        rows = own[part].shape[0]
        mine = pl.ds(pl.multiple_of(origin((0, 0, 0)) * rows, rows), rows)
        local.append(pltpu.make_async_copy(own[part], full[part].at[mine], local_sem.at[part]))
    mine = pl.ds(pl.multiple_of(t * cols, cols), cols)
    local.append(pltpu.make_async_copy(tok, tok_full.at[:, mine], local_sem.at[parts]))
    for copy in local:
        copy.start()
    for copy in last:
        copy.wait_recv()
    for copy in tok_copies:
        copy.wait()
    for copy in copies:
        copy.wait_send()
    for copy in local:
        copy.wait()


def gather_all(tokens, blocks):
    n_sp, n_fs, n_tp = (lax.axis_size(axis) for axis in ("sp", "fs", "tp"))
    gather = Gather(n_sp, n_fs, len(blocks))
    number = sum(len(sends) for _, _, sends in gather.plan())
    shapes = [jax.ShapeDtypeStruct((n_sp * n_fs * b.shape[0], b.shape[1]), b.dtype) for b in blocks]
    shapes.append(jax.ShapeDtypeStruct((tokens.shape[0], tokens.shape[1] * n_tp), tokens.dtype))
    return pl.pallas_call(
        functools.partial(gather_kernel, gather, n_tp),
        out_shape=shapes,
        in_specs=[pl.BlockSpec(memory_space=pltpu.VMEM)] * (len(blocks) + 1),
        out_specs=[pl.BlockSpec(memory_space=pl.ANY)] * len(shapes),
        scratch_shapes=[
            pltpu.SemaphoreType.DMA((number,)),
            pltpu.SemaphoreType.DMA((len(blocks) * n_sp * n_fs,)),
            pltpu.SemaphoreType.DMA((len(blocks) + 1,)),
            pltpu.SemaphoreType.DMA((n_tp,)),
            pltpu.SemaphoreType.DMA((n_tp,)),
        ],
        compiler_params=pltpu.CompilerParams(collective_id=0, has_side_effects=True),
    )(*blocks, tokens)


def out_kernel(n_tp, chunks, mix, w_out, out, outbox, inbox, send_sem, recv_sem):
    s, f, t = lax.axis_index("sp"), lax.axis_index("fs"), lax.axis_index("tp")
    rows = out.shape[0]
    step = rows // chunks
    peers = [(s, f, lax.rem(t + k, n_tp)) for k in range(1, n_tp)]
    barrier = pltpu.get_barrier_semaphore()
    for peer in peers:
        pl.semaphore_signal(barrier, inc=1, device_id=peer, device_id_type=MESH)
    pl.semaphore_wait(barrier, n_tp - 1)

    def partial(owner, chunk):
        first = pl.multiple_of(owner * rows + chunk * step, step)
        return lax.dot_general(
            mix[pl.ds(first, step), :],
            w_out[...],
            (((1,), (1,)), ((), ())),
            preferred_element_type=jnp.float32,
        ).astype(jnp.bfloat16)

    copies = []
    for chunk in range(chunks):
        here = pl.ds(chunk * step, step)
        for k, peer in enumerate(peers):
            outbox[k, here] = partial(peer[2], chunk)
            copy = pltpu.make_async_remote_copy(
                src_ref=outbox.at[k, here],
                dst_ref=inbox.at[k, here],
                send_sem=send_sem.at[k, chunk],
                recv_sem=recv_sem.at[k, chunk],
                device_id=peer,
                device_id_type=MESH,
            )
            copy.start()
            copies.append(copy)
    for chunk in range(chunks):
        out[pl.ds(chunk * step, step)] = partial(t, chunk)
    for chunk in range(chunks):
        here = pl.ds(chunk * step, step)
        total = out[here].astype(jnp.float32)
        for k in range(n_tp - 1):
            copies[chunk * (n_tp - 1) + k].wait_recv()
            total = total + inbox[k, here].astype(jnp.float32)
        out[here] = total.astype(out.dtype)
    for copy in copies:
        copy.wait_send()


def project_out(mixers, w_out):
    n_tp = lax.axis_size("tp")
    rows, width = mixers.shape[0] // n_tp, w_out.shape[0]
    chunks = 4
    return pl.pallas_call(
        functools.partial(out_kernel, n_tp, chunks),
        out_shape=jax.ShapeDtypeStruct((rows, width), jnp.bfloat16),
        in_specs=[pl.BlockSpec(memory_space=pltpu.VMEM)] * 2,
        out_specs=pl.BlockSpec(memory_space=pltpu.VMEM),
        scratch_shapes=[
            pltpu.VMEM((n_tp - 1, rows, width), jnp.bfloat16),
            pltpu.VMEM((n_tp - 1, rows, width), jnp.bfloat16),
            pltpu.SemaphoreType.DMA((n_tp - 1, chunks)),
            pltpu.SemaphoreType.DMA((n_tp - 1, chunks)),
        ],
        compiler_params=pltpu.CompilerParams(collective_id=1, has_side_effects=True),
    )(mixers, w_out)


def shifted(block, axis, distance):
    devices = range(lax.axis_size(axis))
    route = [(i - distance, i) for i in devices if i - distance in devices]
    return lax.ppermute(block, axis, route)


def norm_rows(tokens, norm_gain):
    values = tokens.astype(jnp.float32)
    average = jnp.mean(values, axis=-1, keepdims=True)
    centred = values - average
    variance = jnp.mean(centred * centred, axis=-1, keepdims=True)
    return (centred * lax.rsqrt(variance + 1e-05) * norm_gain).astype(jnp.bfloat16)


def attend(queries, keys_values, earlier_rows, sink_logits, head_base, row_base):
    row_total = queries.shape[0]
    kv_cols = keys_values.shape[1] // 2
    kv_here = kv_cols // HEAD
    heads_here = queries.shape[1] // HEAD
    group = heads_here // kv_here
    keys_all = jnp.concatenate([earlier_rows, keys_values], axis=0)
    block_rows = min(512, row_total)
    head_ids = head_base + jnp.arange(heads_here, dtype=jnp.int32)
    slopes = jnp.exp2(-8.0 * (head_ids + 1).astype(jnp.float32) / HEADS).reshape(kv_here, group)[
        :, :, None, None
    ]
    sinks = sink_logits.reshape(kv_here, group)[:, :, None, None]
    row_ids = jnp.arange(block_rows, dtype=jnp.int32)[:, None]
    col_ids = jnp.arange(block_rows + WINDOW, dtype=jnp.int32)[None, :]
    distance = WINDOW + row_ids - col_ids
    outputs = []
    for block in range(row_total // block_rows):
        first_row = block * block_rows
        query_block = queries[first_row : first_row + block_rows].reshape(
            block_rows, kv_here, group, HEAD
        )
        band = keys_all[first_row : first_row + block_rows + WINDOW]
        band_keys = band[:, :kv_cols].reshape(block_rows + WINDOW, kv_here, HEAD)
        band_values = band[:, kv_cols:].reshape(block_rows + WINDOW, kv_here, HEAD)
        scores = jnp.einsum(
            "qkgd,skd->kgqs", query_block, band_keys, preferred_element_type=jnp.float32
        ) * HEAD ** (-0.5)
        scores = scores - slopes * distance.astype(jnp.float32)
        key_place = row_base + first_row - WINDOW + col_ids
        keep = (distance >= 0) & (distance < WINDOW) & (key_place >= 0)
        scores = jnp.where(keep, scores, -jnp.inf)
        highest = jnp.maximum(jnp.max(scores, axis=-1, keepdims=True), sinks)
        raised = jnp.exp(scores - highest)
        denominator = jnp.sum(raised, axis=-1, keepdims=True) + jnp.exp(sinks - highest)
        weights = (raised / denominator).astype(jnp.bfloat16)
        mixed = jnp.einsum(
            "kgqs,skd->qkgd", weights, band_values, preferred_element_type=jnp.float32
        )
        outputs.append(mixed.astype(jnp.bfloat16).reshape(block_rows, heads_here * HEAD))
    return jnp.concatenate(outputs, axis=0)


def on_device(
    tokens,
    norm_gain,
    w_query,
    w_key,
    w_value,
    w_conv_in,
    w_conv_b,
    w_conv_c,
    conv_taps,
    sink_logits,
    w_attn_out,
    w_conv_out,
):
    blocks = (
        jnp.concatenate([w_query, w_key, w_value], axis=1),
        jnp.concatenate([w_conv_in, w_conv_b], axis=1),
        w_conv_c,
        jnp.concatenate([w_attn_out, w_conv_out], axis=0).T,
    )
    w_qkv, w_conv, w_gate, w_out, gathered = gather_all(tokens[0], blocks)
    normed = norm_rows(gathered, norm_gain)
    row_total = normed.shape[0]
    q_cols, kv_cols, conv_cols = w_query.shape[1], w_key.shape[1], w_conv_in.shape[1]
    qkv = jnp.dot(normed, w_qkv, preferred_element_type=jnp.float32).astype(jnp.bfloat16)
    conv = jnp.dot(normed, w_conv, preferred_element_type=jnp.float32).astype(jnp.bfloat16)
    queries, keys_values = qkv[:, :q_cols], qkv[:, q_cols:]
    inner, gate_b = conv[:, :conv_cols], conv[:, conv_cols:]
    gate_c = jnp.dot(normed, w_gate, preferred_element_type=jnp.float32).astype(jnp.bfloat16)
    product = (gate_c.astype(jnp.float32) * inner.astype(jnp.float32)).astype(jnp.bfloat16)
    earlier_kv, earlier_product = shifted(
        (keys_values[row_total - WINDOW :], product[row_total - 2 :]), "sp", 1
    )
    heads_here = queries.shape[1] // HEAD
    head_base = lax.axis_index("tp") * heads_here
    row_base = lax.axis_index("sp") * row_total
    attended = attend(queries, keys_values, earlier_kv, sink_logits, head_base, row_base)
    taps = conv_taps.astype(jnp.float32)
    padded = jnp.concatenate([earlier_product, product], axis=0).astype(jnp.float32)
    filtered = (
        taps[0] * padded[0:row_total]
        + taps[1] * padded[1 : row_total + 1]
        + taps[2] * padded[2 : row_total + 2]
    )
    conv_out = (gate_b.astype(jnp.float32) * filtered).astype(jnp.bfloat16)
    mixers = jnp.concatenate([attended, conv_out], axis=1)
    summed = project_out(mixers, w_out)
    return summed[None]


def solution(mesh):
    placed = (
        P("fs", "sp", "tp"),
        P(),
        P(("sp", "fs"), "tp"),
        P(("sp", "fs"), "tp"),
        P(("sp", "fs"), "tp"),
        P(("sp", "fs"), "tp"),
        P(("sp", "fs"), "tp"),
        P(("sp", "fs"), "tp"),
        P(None, "tp"),
        P("tp"),
        P("tp", ("sp", "fs")),
        P("tp", ("sp", "fs")),
    )
    return jax.shard_map(
        on_device,
        mesh=mesh,
        in_specs=placed,
        out_specs=P("fs", ("sp", "tp"), None),
        check_vma=False,
    )
```
